32 devices in a mesh: fs: 8 (over z, x), tp: 4 (over y, core).
Axes of the slice: x: 2, y: 2, z: 4, core: 2. Of those that a mesh axis runs over, the one named last changes fastest.
Arguments:
- prompts: bfloat16 [4, 1024, 2048], P('tp'), may hold values from -6 to 6
- gain_first: float32 [2048], P('fs'), may hold values from 0.1 to 1.9
- gate_first: float32 [2048, 5632], P('fs', 'tp'), may hold values from -0.125 to 0.125
- up_first: float32 [2048, 5632], P('fs', 'tp'), may hold values from -0.125 to 0.125
- down_first: float32 [5632, 2048], P('fs', 'tp'), may hold values from -0.078125 to 0.078125
- gain_second: float32 [2048], P('fs'), may hold values from 0.1 to 1.9
- gate_second: float32 [2048, 5632], P('fs', 'tp'), may hold values from -0.125 to 0.125
- up_second: float32 [2048, 5632], P('fs', 'tp'), may hold values from -0.125 to 0.125
- down_second: float32 [5632, 2048], P('fs', 'tp'), may hold values from -0.078125 to 0.078125
Outputs:
- served_gate_first: bfloat16 [2048, 5632], P(None, 'fs')
- served_up_first: bfloat16 [2048, 5632], P(None, 'fs')
- served_down_first: bfloat16 [5632, 2048], P('fs')
- served_gate_second: bfloat16 [2048, 5632], P(None, 'fs')
- served_up_second: bfloat16 [2048, 5632], P(None, 'fs')
- served_down_second: bfloat16 [5632, 2048], P('fs')
- prompt_states: bfloat16 [4, 1024, 2048], P('tp', 'fs')
The draws below stay inside these ranges and needn't reach their ends.
All inputs are finite; a program needn't handle non-finite values.
Results may differ from the reference program's by a relative error of at most 0.012.
Values may be sent and summed in bfloat16 or wider, within the bound.
A program may use at most 128 MiB of HBM per device.

```python
import jax
import jax.numpy as jnp
from jax import lax

D = 2048
FF = 5632
PLEN = 1024
PROMPTS = 4
N_FS = 8


def levels(rng, dims, cuts, smallest, top_value):
    gain, own = 1.0, jax.random.fold_in(rng, 6)
    for dim, parts in cuts:
        draws = jnp.exp(jax.random.uniform(jax.random.fold_in(own, dim), (parts,), jnp.float32, smallest / len(cuts), top_value / len(cuts)))
        gain = gain * jnp.repeat(draws, dims[dim] // parts).reshape([-1 if axis == dim else 1 for axis in range(len(dims))])
    return gain


def bell_draw(own_key, dims, spread, bound, split=(), held_as=jnp.bfloat16):
    factor_of = levels(own_key, dims, split, -0.22, 0.18) if split else 1.0
    result = jax.random.normal(own_key, dims, jnp.float32) * spread * factor_of
    return jnp.minimum(jnp.maximum(result, -bound), bound).astype(held_as)


def setup_inputs(seed: int = 0) -> dict:
    splits = jax.random.split(jax.random.key(seed), 10)
    prompts = bell_draw(splits[0], (PROMPTS, PLEN, D), 1.0, 6.0, ((0, 4),))
    gain_first = jnp.clip(1.0 + 0.18 * jax.random.normal(splits[1], (D,), jnp.float32), 0.1, 1.9)
    gate_first = bell_draw(splits[2], (D, FF), D ** -0.5, 0.125, ((0, 8), (1, 4)), jnp.float32)
    up_first = bell_draw(splits[3], (D, FF), D ** -0.5, 0.125, ((0, 8), (1, 4)), jnp.float32)
    down_first = bell_draw(splits[4], (FF, D), FF ** -0.5, 0.078125, ((0, 8), (1, 4)), jnp.float32)
    gain_second = jnp.clip(1.0 + 0.18 * jax.random.normal(splits[5], (D,), jnp.float32), 0.1, 1.9)
    gate_second = bell_draw(splits[6], (D, FF), D ** -0.5, 0.125, ((0, 8), (1, 4)), jnp.float32)
    up_second = bell_draw(splits[7], (D, FF), D ** -0.5, 0.125, ((0, 8), (1, 4)), jnp.float32)
    down_second = bell_draw(splits[8], (FF, D), FF ** -0.5, 0.078125, ((0, 8), (1, 4)), jnp.float32)
    return dict(prompts=prompts, gain_first=gain_first, gate_first=gate_first, up_first=up_first, down_first=down_first, gain_second=gain_second, gate_second=gate_second, up_second=up_second, down_second=down_second)


def normalize(row_block):
    widened = row_block.astype(jnp.float32)
    scaled = widened * lax.rsqrt(lax.optimization_barrier(jnp.mean(widened * widened, axis=-1, keepdims=True)) + 1e-06)
    return scaled.astype(jnp.bfloat16)

def block_sum(active, down_rows):
    unit_count = active.shape[1] // N_FS

    def advance(running, block_index):
        left_cols = lax.dynamic_slice_in_dim(active, block_index * unit_count, unit_count, 1)
        right_rows = lax.dynamic_slice_in_dim(down_rows, block_index * unit_count, unit_count, 0)
        partial_sum = jnp.dot(left_cols, right_rows, preferred_element_type=jnp.float32).astype(jnp.bfloat16)
        partial_sum = lax.optimization_barrier(partial_sum)
        return (running + partial_sum.astype(jnp.float32), None)
    start_sum = jnp.zeros((active.shape[0], down_rows.shape[1]), jnp.float32)
    running, _ = lax.scan(advance, start_sum, jnp.arange(N_FS, dtype=jnp.int32))
    return running

def half_step(tokens_in, gate_cols, up_cols, down_rows):
    normed = normalize(tokens_in)
    gate_val = jnp.dot(normed, gate_cols, preferred_element_type=jnp.float32)
    up_val = jnp.dot(normed, up_cols, preferred_element_type=jnp.float32)
    active = (jax.nn.silu(gate_val) * up_val).astype(jnp.bfloat16)
    branch = block_sum(active, down_rows)
    return (tokens_in.astype(jnp.float32) + 0.5 * branch).astype(jnp.bfloat16)

def reference(prompts, gain_first, gate_first, up_first, down_first, gain_second, gate_second, up_second, down_second):
    served_gate_first = (gain_first[:, None] * gate_first).astype(jnp.bfloat16)
    served_up_first = (gain_first[:, None] * up_first).astype(jnp.bfloat16)
    served_gate_second = (gain_second[:, None] * gate_second).astype(jnp.bfloat16)
    served_up_second = (gain_second[:, None] * up_second).astype(jnp.bfloat16)
    served_down_first = down_first.astype(jnp.bfloat16)
    served_down_second = down_second.astype(jnp.bfloat16)
    tokens_in = prompts.reshape(-1, prompts.shape[-1])
    middle = half_step(tokens_in, served_gate_first, served_up_first, served_down_first)
    finished = half_step(middle, served_gate_second, served_up_second, served_down_second)
    return (served_gate_first, served_up_first, served_down_first, served_gate_second, served_up_second, served_down_second, finished.reshape(prompts.shape))
```

```python
import functools

import jax
import jax.numpy as jnp
from jax import lax
from jax.experimental import pallas as pl
from jax.experimental.pallas import tpu as pltpu
from jax.sharding import PartitionSpec as P

CORES = 2


def normalize(row_block):
    widened = row_block.astype(jnp.float32)
    scaled = widened * lax.rsqrt(jnp.mean(widened * widened, axis=-1, keepdims=True) + 1e-06)
    return scaled.astype(jnp.bfloat16)


def activate(normed, gate_cols, up_cols):
    gate_val = jnp.dot(normed, gate_cols, preferred_element_type=jnp.float32)
    up_val = jnp.dot(normed, up_cols, preferred_element_type=jnp.float32)
    return (jax.nn.silu(gate_val) * up_val).astype(jnp.bfloat16)


def partner(index, step, count):
    if count & (count - 1):
        return (index + step) % count
    result, bit = 0, 1
    while bit < count:
        result = result + ((index // bit + step // bit) % 2) * bit
        bit *= 2
    return result


def exchange_kernel(n_fs, n_tp, has_down, *refs):
    if has_down:
        (gu, dn, gu_out, dn_out, send_a, recv_a, send_y, recv_y, send_m, recv_m,
         dn_local, dn_send_y, dn_recv_y, dn_send_m, dn_recv_m) = refs
    else:
        gu, gu_out, send_a, recv_a, send_y, recv_y, send_m, recv_m = refs
    per = n_fs // n_tp
    n_y = n_tp // CORES
    rows = gu.shape[2]
    part = rows // n_tp
    me_f, me_t = lax.axis_index("fs"), lax.axis_index("tp")
    my_y, my_c = me_t // CORES, me_t % CORES
    mate = my_y * CORES + (1 - my_c)
    holder = me_f // per
    is_self = holder == me_t

    def peer_y(step):
        return (my_y + step) % n_y

    def window(f, q):
        return gu_out.at[:, pl.ds(pl.multiple_of(f * rows + q * part, part), part), :]

    def remote(src, dst, send, recv, f, t):
        return pltpu.make_async_remote_copy(
            src_ref=src, dst_ref=dst, send_sem=send, recv_sem=recv,
            device_id={"fs": f, "tp": t}, device_id_type=pl.DeviceIdType.MESH,
        )

    barrier = pltpu.get_barrier_semaphore()

    def greet(f, t):
        pl.semaphore_signal(
            barrier, inc=1, device_id={"fs": f, "tp": t}, device_id_type=pl.DeviceIdType.MESH
        )

    for step in range(n_fs):
        f = partner(me_f, step, n_fs)
        if step == 0:
            @pl.when(jnp.logical_not(is_self))
            def _():
                greet(f, holder)
        else:
            greet(f, holder)
    for step in range(1, n_y):
        greet(me_f, peer_y(step) * CORES + my_c)
    greet(me_f, mate)
    pl.semaphore_wait(barrier, per * n_tp + n_y - jnp.where(is_self, 1, 0))

    def first(i, step):
        q = (me_t + step) % n_tp
        f = me_t * per + i
        src = gu.at[:, i, pl.ds(pl.multiple_of(q * part, part), part), :]
        dst = window(me_f, q)
        copy = remote(src, dst, send_a.at[i * n_tp + step], recv_a.at[me_f], f, q)
        return copy, src, dst, f == me_f

    for step in range(n_tp - 1, -1, -1):
        for i in range(per):
            copy, src, dst, here = first(i, step)
            if step == 0:
                @pl.when(here)
                def _():
                    pltpu.make_async_copy(src, dst, recv_a.at[me_f]).start()

                @pl.when(jnp.logical_not(here))
                def _():
                    copy.start()
            else:
                copy.start()

    if has_down:
        width = dn.shape[1]

        def columns(t):
            return dn_out.at[:, pl.ds(pl.multiple_of(t * width, 128), width)]

        keep = pltpu.make_async_copy(dn, columns(me_t), dn_local)
        keep.start()
        dn_sends = []
        for step in range(1, n_y):
            dn_sends.append(remote(dn, columns(me_t), dn_send_y.at[step], dn_recv_y.at[my_y],
                                   me_f, peer_y(step) * CORES + my_c))
        dn_sends.append(remote(dn, columns(me_t), dn_send_m.at[0], dn_recv_m.at[my_y], me_f, mate))
        for copy in dn_sends:
            copy.start()

    sends = []
    for step in range(n_fs):
        f = partner(me_f, step, n_fs)
        piece = window(f, me_t)
        remote(piece, piece, send_m.at[0], recv_a.at[f], me_f, mate).wait_recv()
        for hop in range(1, n_y):
            sends.append(remote(piece, piece, send_y.at[(hop - 1) * n_fs + step],
                                recv_y.at[my_y * n_fs + f], me_f, peer_y(hop) * CORES + my_c))
            sends[-1].start()
        sends.append(remote(piece, piece, send_m.at[step], recv_m.at[my_y * n_fs + f], me_f, mate))
        sends[-1].start()

    if has_down:
        for hop in range(1, n_y):
            y = peer_y(hop)
            block = columns(y * CORES + my_c)
            copy = remote(block, block, dn_send_m.at[hop], dn_recv_m.at[y], me_f, mate)
            remote(block, block, dn_send_m.at[hop], dn_recv_y.at[y], me_f, mate).wait_recv()
            copy.start()
            dn_sends.append(copy)

    for step in range(n_fs):
        f = partner(me_f, step, n_fs)
        for hop in range(1, n_y):
            y = peer_y(hop)
            piece = window(f, y * CORES + my_c)
            send = send_m.at[hop * n_fs + step]
            remote(piece, piece, send, recv_y.at[y * n_fs + f], me_f, mate).wait_recv()
            sends.append(remote(piece, piece, send, recv_m.at[y * n_fs + f], me_f, mate))
            sends[-1].start()

    for hop in range(n_y):
        y = peer_y(hop)
        for step in range(n_fs):
            f = partner(me_f, step, n_fs)
            piece = window(f, y * CORES + (1 - my_c))
            remote(piece, piece, send_m.at[0], recv_m.at[y * n_fs + f], me_f, mate).wait_recv()
        if has_down:
            block = columns(y * CORES + (1 - my_c))
            remote(block, block, dn_send_m.at[0], dn_recv_m.at[y], me_f, mate).wait_recv()

    for copy in sends:
        copy.wait_send()
    for i in range(per):
        for step in range(n_tp):
            copy, _, _, here = first(i, step)
            if step == 0:
                @pl.when(jnp.logical_not(here))
                def _():
                    copy.wait_send()
            else:
                copy.wait_send()
    if has_down:
        keep.wait()
        for copy in dn_sends:
            copy.wait_send()


def exchange(stacked, down, collective_id):
    n_fs, n_tp = lax.axis_size("fs"), lax.axis_size("tp")
    n_y = n_tp // CORES
    kinds, per, rows, cols = stacked.shape
    has_down = down is not None
    dma = pltpu.SemaphoreType.DMA
    scratch = [dma((per * n_tp,)), dma((n_fs,)), dma((n_y * n_fs,)), dma((n_y * n_fs,)),
               dma((n_y * n_fs,)), dma((n_y * n_fs,))]
    outs = [jax.ShapeDtypeStruct((kinds, n_fs * rows, cols), stacked.dtype)]
    operands = [stacked]
    if has_down:
        scratch += [dma, dma((n_y,)), dma((n_y,)), dma((n_y,)), dma((n_y,))]
        outs.append(jax.ShapeDtypeStruct((down.shape[0], n_tp * down.shape[1]), down.dtype))
        operands.append(down)
    total = sum(out.size * 2 for out in outs)
    return pl.pallas_call(
        functools.partial(exchange_kernel, n_fs, n_tp, has_down),
        out_shape=outs,
        in_specs=[pl.BlockSpec(memory_space=pltpu.VMEM)] * len(operands),
        out_specs=[pl.BlockSpec(memory_space=pl.ANY)] * len(outs),
        scratch_shapes=scratch,
        compiler_params=pltpu.CompilerParams(
            collective_id=collective_id, has_side_effects=True, vmem_limit_bytes=16 * 2**20
        ),
        cost_estimate=pl.CostEstimate(flops=0, bytes_accessed=total * 24, transcendentals=0),
    )(*operands)


def per_device(
    prompts,
    gain_first,
    gate_first,
    up_first,
    down_first,
    gain_second,
    gate_second,
    up_second,
    down_second,
):
    per = lax.axis_size("fs") // lax.axis_size("tp")

    def fold(gain, *matrices):
        blocks = []
        for matrix in matrices:
            folded = (gain[:, None] * matrix).astype(jnp.bfloat16)
            width = folded.shape[1] // per
            blocks.append(jnp.stack([folded[:, i * width:(i + 1) * width] for i in range(per)]))
        return jnp.stack(blocks)

    served_a, down_a = exchange(
        fold(gain_first, gate_first, up_first), down_first.astype(jnp.bfloat16), 0
    )
    gate_a, up_a = served_a[0], served_a[1]

    tokens_in = prompts.reshape(-1, prompts.shape[-1])
    share = tokens_in.shape[0] // lax.axis_size("fs")
    act_first = activate(normalize(tokens_in), gate_a, up_a)
    branch = jnp.dot(act_first, down_a, preferred_element_type=jnp.float32).astype(jnp.bfloat16)

    stack_b = fold(gain_second, gate_second, up_second)
    round_b = down_second.astype(jnp.bfloat16)
    stack_b, round_b, branch = lax.optimization_barrier((stack_b, round_b, branch))
    gate_stack_b, down_b = exchange(stack_b[:1], round_b, 1)
    summed = lax.psum_scatter(branch, "fs", scatter_dimension=0, tiled=True)
    summed, gate_stack_b, down_b = lax.optimization_barrier((summed, gate_stack_b, down_b))
    summed = summed.astype(jnp.float32)
    own_rows = lax.dynamic_slice_in_dim(tokens_in, lax.axis_index("fs") * share, share, 0)
    middle = (own_rows.astype(jnp.float32) + 0.5 * summed).astype(jnp.bfloat16)
    normed = normalize(middle)
    up_in, normed = lax.optimization_barrier((stack_b[1:], normed))
    (up_stack_b,) = exchange(up_in, None, 2)
    gathered = lax.all_gather(normed, "fs", axis=0, tiled=True)
    gate_b, up_b = gate_stack_b[0], up_stack_b[0]
    act_second = activate(gathered, gate_b, up_b)
    final_sum = lax.psum_scatter(
        jnp.dot(act_second, down_b, preferred_element_type=jnp.float32).astype(jnp.bfloat16),
        "fs",
        scatter_dimension=0,
        tiled=True,
    ).astype(jnp.float32)
    finished = (middle.astype(jnp.float32) + 0.5 * final_sum).astype(jnp.bfloat16)
    return (
        gate_a,
        up_a,
        down_a,
        gate_b,
        up_b,
        down_b,
        finished.reshape(prompts.shape[0], share, prompts.shape[-1]),
    )


def solution(mesh):
    in_specs = (
        P("tp", None, None),
        P("fs"),
        P("fs", "tp"),
        P("fs", "tp"),
        P("fs", "tp"),
        P("fs"),
        P("fs", "tp"),
        P("fs", "tp"),
        P("fs", "tp"),
    )
    out_specs = (
        P(None, "fs"),
        P(None, "fs"),
        P("fs", None),
        P(None, "fs"),
        P(None, "fs"),
        P("fs", None),
        P("tp", "fs", None),
    )
    return jax.shard_map(
        per_device, mesh=mesh, in_specs=in_specs, out_specs=out_specs, check_vma=False
    )
```

```python
import functools

import jax
import jax.numpy as jnp
from jax import lax
from jax.experimental import pallas as pl
from jax.experimental.pallas import tpu as pltpu
from jax.sharding import PartitionSpec as P

CORES = 2


def normalize(row_block):
    widened = row_block.astype(jnp.float32)
    scaled = widened * lax.rsqrt(jnp.mean(widened * widened, axis=-1, keepdims=True) + 1e-06)
    return scaled.astype(jnp.bfloat16)


def activate(normed, gate_cols, up_cols):
    gate_val = jnp.dot(normed, gate_cols, preferred_element_type=jnp.float32)
    up_val = jnp.dot(normed, up_cols, preferred_element_type=jnp.float32)
    return (jax.nn.silu(gate_val) * up_val).astype(jnp.bfloat16)


def partner(index, step, count):
    if count & (count - 1):
        return (index + step) % count
    result, bit = 0, 1
    while bit < count:
        result = result + ((index // bit + step // bit) % 2) * bit
        bit *= 2
    return result


def exchange_kernel(n_fs, n_tp, has_down, *refs):
    if has_down:
        (gu, dn, gu_out, dn_out, send_a, recv_a, send_y, recv_y, send_m, recv_m,
         dn_local, dn_send_y, dn_recv_y, dn_send_m, dn_recv_m) = refs
    else:
        gu, gu_out, send_a, recv_a, send_y, recv_y, send_m, recv_m = refs
    per = n_fs // n_tp
    n_y = n_tp // CORES
    rows = gu.shape[2]
    part = rows // n_tp
    me_f, me_t = lax.axis_index("fs"), lax.axis_index("tp")
    my_y, my_c = me_t // CORES, me_t % CORES
    mate = my_y * CORES + (1 - my_c)
    holder = me_f // per
    is_self = holder == me_t

    def peer_y(step):
        return (my_y + step) % n_y

    def window(f, q):
        return gu_out.at[:, pl.ds(pl.multiple_of(f * rows + q * part, part), part), :]

    def remote(src, dst, send, recv, f, t):
        return pltpu.make_async_remote_copy(
            src_ref=src, dst_ref=dst, send_sem=send, recv_sem=recv,
            device_id={"fs": f, "tp": t}, device_id_type=pl.DeviceIdType.MESH,
        )

    barrier = pltpu.get_barrier_semaphore()

    def greet(f, t):
        pl.semaphore_signal(
            barrier, inc=1, device_id={"fs": f, "tp": t}, device_id_type=pl.DeviceIdType.MESH
        )

    for step in range(n_fs):
        f = partner(me_f, step, n_fs)
        if step == 0:
            @pl.when(jnp.logical_not(is_self))
            def _():
                greet(f, holder)
        else:
            greet(f, holder)
    for step in range(1, n_y):
        greet(me_f, peer_y(step) * CORES + my_c)
    greet(me_f, mate)
    pl.semaphore_wait(barrier, per * n_tp + n_y - jnp.where(is_self, 1, 0))

    def first(i, step):
        q = (me_t + step) % n_tp
        f = me_t * per + i
        src = gu.at[:, i, pl.ds(pl.multiple_of(q * part, part), part), :]
        dst = window(me_f, q)
        copy = remote(src, dst, send_a.at[i * n_tp + step], recv_a.at[me_f], f, q)
        return copy, src, dst, f == me_f

    for step in range(n_tp - 1, -1, -1):
        for i in range(per):
            copy, src, dst, here = first(i, step)
            if step == 0:
                @pl.when(here)
                def _():
                    pltpu.make_async_copy(src, dst, recv_a.at[me_f]).start()

                @pl.when(jnp.logical_not(here))
                def _():
                    copy.start()
            else:
                copy.start()

    if has_down:
        width = dn.shape[1]

        def columns(t):
            return dn_out.at[:, pl.ds(pl.multiple_of(t * width, 128), width)]

        keep = pltpu.make_async_copy(dn, columns(me_t), dn_local)
        keep.start()
        dn_sends = []
        for step in range(1, n_y):
            dn_sends.append(remote(dn, columns(me_t), dn_send_y.at[step], dn_recv_y.at[my_y],
                                   me_f, peer_y(step) * CORES + my_c))
        dn_sends.append(remote(dn, columns(me_t), dn_send_m.at[0], dn_recv_m.at[my_y], me_f, mate))
        for copy in dn_sends:
            copy.start()

    sends = []
    for step in range(n_fs):
        f = partner(me_f, step, n_fs)
        piece = window(f, me_t)
        remote(piece, piece, send_m.at[0], recv_a.at[f], me_f, mate).wait_recv()
        for hop in range(1, n_y):
            sends.append(remote(piece, piece, send_y.at[(hop - 1) * n_fs + step],
                                recv_y.at[my_y * n_fs + f], me_f, peer_y(hop) * CORES + my_c))
            sends[-1].start()
        sends.append(remote(piece, piece, send_m.at[step], recv_m.at[my_y * n_fs + f], me_f, mate))
        sends[-1].start()

    if has_down:
        for hop in range(1, n_y):
            y = peer_y(hop)
            block = columns(y * CORES + my_c)
            copy = remote(block, block, dn_send_m.at[hop], dn_recv_m.at[y], me_f, mate)
            remote(block, block, dn_send_m.at[hop], dn_recv_y.at[y], me_f, mate).wait_recv()
            copy.start()
            dn_sends.append(copy)

    for step in range(n_fs):
        f = partner(me_f, step, n_fs)
        for hop in range(1, n_y):
            y = peer_y(hop)
            piece = window(f, y * CORES + my_c)
            send = send_m.at[hop * n_fs + step]
            remote(piece, piece, send, recv_y.at[y * n_fs + f], me_f, mate).wait_recv()
            sends.append(remote(piece, piece, send, recv_m.at[y * n_fs + f], me_f, mate))
            sends[-1].start()

    for hop in range(n_y):
        y = peer_y(hop)
        for step in range(n_fs):
            f = partner(me_f, step, n_fs)
            piece = window(f, y * CORES + (1 - my_c))
            remote(piece, piece, send_m.at[0], recv_m.at[y * n_fs + f], me_f, mate).wait_recv()
        if has_down:
            block = columns(y * CORES + (1 - my_c))
            remote(block, block, dn_send_m.at[0], dn_recv_m.at[y], me_f, mate).wait_recv()

    for copy in sends:
        copy.wait_send()
    for i in range(per):
        for step in range(n_tp):
            copy, _, _, here = first(i, step)
            if step == 0:
                @pl.when(jnp.logical_not(here))
                def _():
                    copy.wait_send()
            else:
                copy.wait_send()
    if has_down:
        keep.wait()
        for copy in dn_sends:
            copy.wait_send()


def exchange(stacked, down, collective_id):
    n_fs, n_tp = lax.axis_size("fs"), lax.axis_size("tp")
    n_y = n_tp // CORES
    kinds, per, rows, cols = stacked.shape
    has_down = down is not None
    dma = pltpu.SemaphoreType.DMA
    scratch = [dma((per * n_tp,)), dma((n_fs,)), dma((n_y * n_fs,)), dma((n_y * n_fs,)),
               dma((n_y * n_fs,)), dma((n_y * n_fs,))]
    outs = [jax.ShapeDtypeStruct((kinds, n_fs * rows, cols), stacked.dtype)]
    operands = [stacked]
    if has_down:
        scratch += [dma, dma((n_y,)), dma((n_y,)), dma((n_y,)), dma((n_y,))]
        outs.append(jax.ShapeDtypeStruct((down.shape[0], n_tp * down.shape[1]), down.dtype))
        operands.append(down)
    total = sum(out.size * 2 for out in outs)
    return pl.pallas_call(
        functools.partial(exchange_kernel, n_fs, n_tp, has_down),
        out_shape=outs,
        in_specs=[pl.BlockSpec(memory_space=pltpu.VMEM)] * len(operands),
        out_specs=[pl.BlockSpec(memory_space=pl.ANY)] * len(outs),
        scratch_shapes=scratch,
        compiler_params=pltpu.CompilerParams(
            collective_id=collective_id, has_side_effects=True, vmem_limit_bytes=16 * 2**20
        ),
        cost_estimate=pl.CostEstimate(flops=0, bytes_accessed=total * 24, transcendentals=0),
    )(*operands)


def gather_kernel(n_z, n_x, cuts, blk, out, local, send_z, recv_z, send_x, recv_x):
    share = blk.shape[0]
    part = share // cuts
    me_f, me_t = lax.axis_index("fs"), lax.axis_index("tp")
    z, x = me_f // n_x, me_f % n_x

    def window(zs, xs, s):
        start = (zs * n_x + xs) * share + s * part
        return out.at[pl.ds(pl.multiple_of(start, part), part), :]

    def remote(src, dst, send, recv, f):
        return pltpu.make_async_remote_copy(
            src_ref=src, dst_ref=dst, send_sem=send, recv_sem=recv,
            device_id={"fs": f, "tp": me_t}, device_id_type=pl.DeviceIdType.MESH,
        )

    has_next = (z < n_z - 1, z > 0)
    toward = (1, -1)
    barrier = pltpu.get_barrier_semaphore()

    def greet(f):
        pl.semaphore_signal(
            barrier, inc=1, device_id={"fs": f, "tp": me_t}, device_id_type=pl.DeviceIdType.MESH
        )

    for way in range(2):
        @pl.when(has_next[way])
        def _():
            greet(me_f + toward[way] * n_x)
    for off in range(1, n_x):
        greet(z * n_x + (x + off) % n_x)
    pl.semaphore_wait(
        barrier, n_x - 1 + jnp.where(has_next[0], 1, 0) + jnp.where(has_next[1], 1, 0)
    )

    def source(k, s, zs):
        piece = window(zs, x, s)
        return (blk.at[pl.ds(s * part, part), :] if k == 0 else piece), piece

    def along_z(way, k, s, zs):
        src, piece = source(k, s, zs)
        return remote(src, piece, send_z.at[(way * n_z + k) * cuts + s],
                      recv_z.at[(way * n_z + k + 1) * cuts + s], me_f + toward[way] * n_x)

    def along_x(off, k, s, zs):
        src, piece = source(k, s, zs)
        return remote(src, piece, send_x.at[(off * n_z + zs) * cuts + s],
                      recv_x.at[(off * n_z + zs) * cuts + s], z * n_x + (x + off) % n_x)

    keep = pltpu.make_async_copy(blk, out.at[pl.ds(pl.multiple_of(me_f * share, share), share), :],
                                 local)
    keep.start()
    for s in range(cuts):
        for way in range(2):
            @pl.when(has_next[way])
            def _():
                along_z(way, 0, s, z).start()
        for off in range(1, n_x):
            along_x(off, 0, s, z).start()

    def each_arrival(body):
        for k in range(1, n_z):
            for s in range(cuts):
                for way in range(2):
                    zs = z - k * toward[way]
                    inside = (z >= k) if way == 0 else (z + k < n_z)

                    @pl.when(inside)
                    def _():
                        body(way, k, s, zs)

    def pass_on(way, k, s, zs):
        piece = window(zs, x, s)
        remote(piece, piece, send_z.at[0], recv_z.at[(way * n_z + k) * cuts + s],
               me_f - toward[way] * n_x).wait_recv()

        @pl.when(has_next[way])
        def _():
            along_z(way, k, s, zs).start()
        for off in range(1, n_x):
            along_x(off, k, s, zs).start()

    each_arrival(pass_on)
    for zs in range(n_z):
        for off in range(1, n_x):
            for s in range(cuts):
                piece = window(zs, (x + n_x - off) % n_x, s)
                remote(piece, piece, send_x.at[0], recv_x.at[(off * n_z + zs) * cuts + s],
                       z * n_x + (x + off) % n_x).wait_recv()

    def sent(way, k, s, zs):
        @pl.when(has_next[way])
        def _():
            along_z(way, k, s, zs).wait_send()
        for off in range(1, n_x):
            along_x(off, k, s, zs).wait_send()

    each_arrival(sent)
    for s in range(cuts):
        for way in range(2):
            @pl.when(has_next[way])
            def _():
                along_z(way, 0, s, z).wait_send()
        for off in range(1, n_x):
            along_x(off, 0, s, z).wait_send()
    keep.wait()


def gather_rows(block, collective_id):
    n_fs = lax.axis_size("fs")
    n_x = lax.axis_size("tp") // CORES
    n_z = n_fs // n_x
    cuts = 2
    dma = pltpu.SemaphoreType.DMA
    return pl.pallas_call(
        functools.partial(gather_kernel, n_z, n_x, cuts),
        out_shape=jax.ShapeDtypeStruct((n_fs * block.shape[0], block.shape[1]), block.dtype),
        in_specs=[pl.BlockSpec(memory_space=pltpu.VMEM)],
        out_specs=pl.BlockSpec(memory_space=pl.ANY),
        scratch_shapes=[dma, dma((2 * (n_z + 1) * cuts,)), dma((2 * (n_z + 1) * cuts,)),
                        dma((n_x * n_z * cuts,)), dma((n_x * n_z * cuts,))],
        compiler_params=pltpu.CompilerParams(
            collective_id=collective_id, has_side_effects=True, vmem_limit_bytes=16 * 2**20
        ),
    )(block)


def per_device(
    prompts,
    gain_first,
    gate_first,
    up_first,
    down_first,
    gain_second,
    gate_second,
    up_second,
    down_second,
):
    per = lax.axis_size("fs") // lax.axis_size("tp")

    def fold(gain, *matrices):
        blocks = []
        for matrix in matrices:
            folded = (gain[:, None] * matrix).astype(jnp.bfloat16)
            width = folded.shape[1] // per
            blocks.append(jnp.stack([folded[:, i * width:(i + 1) * width] for i in range(per)]))
        return jnp.stack(blocks)

    served_a, down_a = exchange(
        fold(gain_first, gate_first, up_first), down_first.astype(jnp.bfloat16), 0
    )
    gate_a, up_a = served_a[0], served_a[1]

    tokens_in = prompts.reshape(-1, prompts.shape[-1])
    share = tokens_in.shape[0] // lax.axis_size("fs")
    act_first = activate(normalize(tokens_in), gate_a, up_a)
    branch = jnp.dot(act_first, down_a, preferred_element_type=jnp.float32).astype(jnp.bfloat16)

    stack_b = fold(gain_second, gate_second, up_second)
    round_b = down_second.astype(jnp.bfloat16)
    stack_b, round_b, branch = lax.optimization_barrier((stack_b, round_b, branch))
    served_b, down_b = exchange(stack_b, round_b, 1)
    summed = lax.psum_scatter(branch, "fs", scatter_dimension=0, tiled=True)
    summed, served_b, down_b = lax.optimization_barrier((summed, served_b, down_b))
    summed = summed.astype(jnp.float32)
    own_rows = lax.dynamic_slice_in_dim(tokens_in, lax.axis_index("fs") * share, share, 0)
    middle = (own_rows.astype(jnp.float32) + 0.5 * summed).astype(jnp.bfloat16)
    gathered = gather_rows(normalize(middle), 2)
    gate_b, up_b = served_b[0], served_b[1]
    act_second = activate(gathered, gate_b, up_b)
    final_sum = lax.psum_scatter(
        jnp.dot(act_second, down_b, preferred_element_type=jnp.float32).astype(jnp.bfloat16),
        "fs",
        scatter_dimension=0,
        tiled=True,
    ).astype(jnp.float32)
    finished = (middle.astype(jnp.float32) + 0.5 * final_sum).astype(jnp.bfloat16)
    return (
        gate_a,
        up_a,
        down_a,
        gate_b,
        up_b,
        down_b,
        finished.reshape(prompts.shape[0], share, prompts.shape[-1]),
    )


def solution(mesh):
    in_specs = (
        P("tp", None, None),
        P("fs"),
        P("fs", "tp"),
        P("fs", "tp"),
        P("fs", "tp"),
        P("fs"),
        P("fs", "tp"),
        P("fs", "tp"),
        P("fs", "tp"),
    )
    out_specs = (
        P(None, "fs"),
        P(None, "fs"),
        P("fs", None),
        P(None, "fs"),
        P(None, "fs"),
        P("fs", None),
        P("tp", "fs", None),
    )
    return jax.shard_map(
        per_device, mesh=mesh, in_specs=in_specs, out_specs=out_specs, check_vma=False
    )
```
